128 devices in a mesh: sp: 16 (over z, x), tp: 8 (over y, core).
Axes of the slice: x: 4, y: 4, z: 4, core: 2. Of those that a mesh axis runs over, the one named last changes fastest.
Arguments:
- queries: bfloat16 [8192, 3072], P('sp', 'tp'), may hold values from -6 to 6
- latent: bfloat16 [8192, 1024], P('sp'), may hold values from -6 to 6
- rope_key: bfloat16 [8192, 64], P('sp'), may hold values from -6 to 6
- key_weight: bfloat16 [1024, 2048], P(None, 'tp'), as said below
- value_weight: bfloat16 [1024, 2048], P(None, 'tp'), as said below
- log_sums: float32 [16, 8192], P('tp', 'sp'), as said below
- attn_out: bfloat16 [8192, 2048], P('sp', 'tp'), as said below
- out_grad: bfloat16 [8192, 2048], P('sp', 'tp'), may hold values from -6 to 6
Outputs:
- d_queries: bfloat16 [8192, 3072], P('sp', 'tp')
- d_latent: float32 [8192, 1024], P('sp')
- d_rope: float32 [8192, 64], P('sp')
- d_value_weight: float32 [1024, 2048], P('sp', 'tp')
The draws below stay inside these ranges and needn't reach their ends.
Inputs may be any that keep to these rules, and one draw needn't show every extreme that they name: `key_weight`: independent entries of order one multiplied by 1024^(-1/2). `value_weight`: independent entries of order one multiplied by 1024^(-1/2). log_sums[h, i] is the logarithm of the sum over j <= i of exp(scores[h, i, j]) of the forward pass. attn_out is the forward pass output: head h of row i is the sum over j <= i of exp(scores - log_sums) rounded to bfloat16, times head h of values row j, rounded to bfloat16.
All inputs are finite; a program needn't handle non-finite values.
Results may differ from the reference program's by a relative error of at most 0.018.
Values may be sent and summed in bfloat16 or wider, within the bound.
No kernel may reach another device: no remote copies, remote signals or barrier semaphores. Data moves between devices by JAX's collectives and lax.ppermute only.
A program may use at most 192 MiB of HBM per device.

```python
import jax
import jax.numpy as jnp
from jax import lax

HEADS = 16
NOPE = 128
ROPE = 64
VDIM = 128
LATENT = 1024
TOKENS = 8192


def rough_normal(key, shape):
    return jnp.clip(jax.random.normal(key, shape, jnp.float32), -6.0, 6.0)


def base_inputs(key):
    queries = rough_normal(jax.random.fold_in(key, 101), (TOKENS, HEADS * (NOPE + ROPE)))
    latent = rough_normal(jax.random.fold_in(key, 102), (TOKENS, LATENT))
    rope_key = rough_normal(jax.random.fold_in(key, 103), (TOKENS, ROPE))
    key_weight = rough_normal(jax.random.fold_in(key, 104), (LATENT, HEADS * NOPE)) * LATENT ** (-0.5)
    value_weight = rough_normal(jax.random.fold_in(key, 105), (LATENT, HEADS * VDIM)) * LATENT ** (-0.5)
    return (queries.astype(jnp.bfloat16), latent.astype(jnp.bfloat16), rope_key.astype(jnp.bfloat16), key_weight.astype(jnp.bfloat16), value_weight.astype(jnp.bfloat16))


def forward_outputs(key):
    queries, latent, rope_key, key_weight, value_weight = base_inputs(key)
    head_width = NOPE + ROPE
    score_scale = head_width ** (-0.5)
    key_nope = jnp.dot(latent, key_weight, preferred_element_type=jnp.float32).astype(jnp.bfloat16)
    values = jnp.dot(latent, value_weight, preferred_element_type=jnp.float32).astype(jnp.bfloat16)
    query_heads = queries.reshape(TOKENS, HEADS, head_width).transpose(1, 0, 2)
    key_heads = key_nope.reshape(TOKENS, HEADS, NOPE).transpose(1, 0, 2)
    value_heads = values.reshape(TOKENS, HEADS, VDIM).transpose(1, 0, 2)
    positions = jnp.arange(TOKENS, dtype=jnp.int32)
    causal = positions[None, :] <= positions[:, None]

    def one_head(operands):
        query_h, key_h, value_h = operands
        scores = score_scale * (jnp.dot(query_h[:, :NOPE], key_h.T, preferred_element_type=jnp.float32) + jnp.dot(query_h[:, NOPE:], rope_key.T, preferred_element_type=jnp.float32))
        masked = jnp.where(causal, scores, -jnp.inf)
        log_sum = jax.nn.logsumexp(masked, axis=1)
        attn_probs = jnp.exp(masked - log_sum[:, None]).astype(jnp.bfloat16)
        return (log_sum, jnp.dot(attn_probs, value_h, preferred_element_type=jnp.float32).astype(jnp.bfloat16))
    log_sums, out_heads = lax.map(one_head, (query_heads, key_heads, value_heads))
    return (log_sums, out_heads.transpose(1, 0, 2).reshape(TOKENS, HEADS * VDIM))


def draw_queries(key, part):
    return base_inputs(key)[0]


def draw_latent(key, part):
    return base_inputs(key)[1]


def draw_rope_key(key, part):
    return base_inputs(key)[2]


def draw_key_weight(key, part):
    return base_inputs(key)[3]


def draw_value_weight(key, part):
    return base_inputs(key)[4]


def draw_log_sums(key, part):
    return forward_outputs(key)[0]


def draw_attn_out(key, part):
    return forward_outputs(key)[1]


def strengthened(result, key, source, target, shards_of, factor):
    owner, partner = [(jnp.arange(result.shape[dim]) // (result.shape[dim] // shards_of)).reshape([-1 if axis == dim else 1 for axis in range(result.ndim)]) for dim in (source, target)]
    chosen = jax.random.permutation(key, shards_of)[partner]
    strong = (owner == chosen) | (owner == (partner + shards_of // 2) % shards_of)
    return jnp.where(strong, factor * result, result)


def shard_levels(own_key, dims, pieces, low, top_value):
    loudness = 1.0
    for axis_at, blocks in pieces:
        steps = jax.random.uniform(jax.random.fold_in(jax.random.fold_in(own_key, 6), axis_at), (blocks,), jnp.float32, low / len(pieces), top_value / len(pieces))
        loudness = loudness * jnp.repeat(jnp.exp(steps), dims[axis_at] // blocks).reshape((-1,) + (1,) * (len(dims) - 1 - axis_at))
    return loudness


def noise_with(rng, extent, deviation, reach, split, heavy, kind=jnp.bfloat16):
    drawn = deviation * jax.random.normal(rng, extent, jnp.float32)
    if split:
        drawn = drawn * shard_levels(rng, extent, split, -0.22, 0.18)
    return jnp.clip(strengthened(drawn, jax.random.fold_in(rng, 3), *heavy), -reach, reach).astype(kind)


def setup_inputs(seed: int = 0) -> dict:
    keys = jax.random.split(jax.random.key(seed), 9)
    return {
        "queries": draw_queries(jax.random.fold_in(keys[8], 71), 0),
        "latent": draw_latent(jax.random.fold_in(keys[8], 71), 0),
        "rope_key": draw_rope_key(jax.random.fold_in(keys[8], 71), 0),
        "key_weight": draw_key_weight(jax.random.fold_in(keys[8], 71), 0),
        "value_weight": draw_value_weight(jax.random.fold_in(keys[8], 71), 0),
        "log_sums": draw_log_sums(jax.random.fold_in(keys[8], 71), 0),
        "attn_out": draw_attn_out(jax.random.fold_in(keys[8], 71), 0),
        "out_grad": noise_with(keys[7], (TOKENS, HEADS * VDIM), 1.0, 6.0, ((0, 16), (1, 8)), (0, 1, 16, 2.0)),
    }


def reference(queries, latent, rope_key, key_weight, value_weight, log_sums, attn_out, out_grad):
    tok_count = queries.shape[0]
    head_width = NOPE + ROPE
    score_scale = head_width ** -0.5
    key_nope = jnp.dot(latent, key_weight, preferred_element_type=jnp.float32).astype(jnp.bfloat16)
    values = jnp.dot(latent, value_weight, preferred_element_type=jnp.float32).astype(jnp.bfloat16)
    query_heads = queries.reshape(tok_count, HEADS, head_width).transpose(1, 0, 2)
    key_heads = key_nope.reshape(tok_count, HEADS, NOPE).transpose(1, 0, 2)
    value_heads = values.reshape(tok_count, HEADS, VDIM).transpose(1, 0, 2)
    grad_heads = out_grad.reshape(tok_count, HEADS, VDIM).transpose(1, 0, 2)
    out_heads = attn_out.reshape(tok_count, HEADS, VDIM).transpose(1, 0, 2)
    row_terms = jnp.sum(out_heads.astype(jnp.float32) * grad_heads.astype(jnp.float32), axis=-1)
    positions = jnp.arange(tok_count, dtype=jnp.int32)
    causal = positions[None, :] <= positions[:, None]

    def one_head(operands):
        query_h, key_h, value_h, grad_h, lse_h, delta_h = operands
        scores = score_scale * (jnp.dot(query_h[:, :NOPE], key_h.T, preferred_element_type=jnp.float32)
                                + jnp.dot(query_h[:, NOPE:], rope_key.T, preferred_element_type=jnp.float32))
        attn_probs = jnp.exp(jnp.where(causal, scores - lse_h[:, None], -1e30))
        probs_b = attn_probs.astype(jnp.bfloat16)
        value_grad = jnp.dot(probs_b.T, grad_h, preferred_element_type=jnp.float32)
        prob_grad = jnp.dot(grad_h, value_h.T, preferred_element_type=jnp.float32)
        score_grad = (attn_probs * (prob_grad - delta_h[:, None])).astype(jnp.bfloat16)
        query_grad = score_scale * jnp.concatenate(
            [jnp.dot(score_grad, key_h, preferred_element_type=jnp.float32),
             jnp.dot(score_grad, rope_key, preferred_element_type=jnp.float32)], axis=1)
        key_grad = score_scale * jnp.dot(score_grad.T, query_h[:, :NOPE], preferred_element_type=jnp.float32)
        rope_grad = score_scale * jnp.dot(score_grad.T, query_h[:, NOPE:], preferred_element_type=jnp.float32)
        return query_grad, key_grad, rope_grad, value_grad

    query_grad, key_grad, rope_grad, value_grad = lax.map(
        one_head, (query_heads, key_heads, value_heads, grad_heads, log_sums, row_terms))
    d_queries = query_grad.transpose(1, 0, 2).reshape(tok_count, HEADS * head_width).astype(jnp.bfloat16)
    key_grad_b = key_grad.transpose(1, 0, 2).reshape(tok_count, HEADS * NOPE).astype(jnp.bfloat16)
    value_grad_b = value_grad.transpose(1, 0, 2).reshape(tok_count, HEADS * VDIM).astype(jnp.bfloat16)
    d_latent = (jnp.dot(key_grad_b, key_weight.T, preferred_element_type=jnp.float32)
                + jnp.dot(value_grad_b, value_weight.T, preferred_element_type=jnp.float32))
    d_rope = jnp.sum(rope_grad, axis=0)
    d_value_weight = jnp.dot(latent.T, value_grad_b, preferred_element_type=jnp.float32)
    return (d_queries, d_latent, d_rope, d_value_weight)
```

```python
import functools

import jax
import jax.numpy as jnp
from jax import lax
from jax.experimental import pallas as pl
from jax.experimental.pallas import tpu as pltpu
from jax.sharding import PartitionSpec as P

NOPE = 128
ROPE = 64
VDIM = 128
WIDTH = NOPE + ROPE
LATENT = 1024
ROWS = 512
SIDE = 4
MSG = 2 * ROWS + ROWS // 2 + 32
KMSG = 2 * ROWS + ROWS // 2
SCALE = WIDTH ** (-0.5)
LOG2E = 1.4426950408889634
SHIFTS = (1, -1, 2)
OUTW = LATENT + 128


f32 = jnp.float32
bf16 = jnp.bfloat16


def nn(a, b):
    return lax.dot_general(a, b, (((1,), (0,)), ((), ())), preferred_element_type=f32)


def nt(a, b):
    return lax.dot_general(a, b, (((1,), (1,)), ((), ())), preferred_element_type=f32)


def tn(a, b):
    return lax.dot_general(a, b, (((0,), (0,)), ((), ())), preferred_element_type=f32)


def x_perm(d):
    return [(z * SIDE + x, z * SIDE + (x + d) % SIDE) for z in range(SIDE) for x in range(SIDE)]


def z_perm(d):
    return [(z * SIDE + x, ((z + d) % SIDE) * SIDE + x) for z in range(SIDE) for x in range(SIDE)]


def y_perm(d):
    return [(2 * y + c, 2 * ((y + d) % SIDE) + c) for y in range(SIDE) for c in range(2)]


def core_perm():
    return [(t, t ^ 1) for t in range(2 * SIDE)]


def place():
    r = lax.axis_index("sp")
    return r // SIDE, r % SIDE


def fold(x):
    half = x.shape[0] // 2
    return jnp.concatenate([x[:half], x[half:]], axis=1)


def unfold(x):
    w = x.shape[1] // 2
    return jnp.concatenate([x[:, :w], x[:, w:]], axis=0)


def three(row):
    hi = row.astype(bf16).astype(f32)
    rest = row - hi
    mid = rest.astype(bf16).astype(f32)
    return hi, mid, rest - mid


def prep_q_body(q_ref, ao_ref, og_ref, ls_ref, qa_ref, qb_ref):
    ones = jnp.ones((8, VDIM), bf16)
    for h, out in enumerate((qa_ref, qb_ref)):
        at = h * WIDTH
        out[0:ROWS, :] = q_ref[:, at : at + NOPE]
        og = og_ref[:, h * VDIM : (h + 1) * VDIM]
        out[ROWS : 2 * ROWS, :] = og
        out[2 * ROWS : KMSG, :] = fold(q_ref[:, at + NOPE : at + WIDTH])
        prod = ao_ref[:, h * VDIM : (h + 1) * VDIM].astype(f32) * og.astype(f32)
        hi = prod.astype(bf16)
        mid = (prod - hi.astype(f32)).astype(bf16)
        delta = (nt(ones, hi) + nt(ones, mid))[0:1]
        lse = ls_ref[h : h + 1, :] * LOG2E
        pieces = []
        for row in three(lse) + three(delta):
            pieces += [row[:, 128 * j : 128 * j + 128] for j in range(ROWS // 128)]
        pieces.append(jnp.zeros((8, 128), f32))
        out[KMSG:MSG, :] = jnp.concatenate(pieces, axis=0).astype(bf16)


def prep_k_body(lat_ref, wk_ref, wv_ref, rope_ref, qb_ref, ka_ref, kb_ref, z1_ref, z2_ref, z3_ref):
    a, _ = place()
    lat = lat_ref[...]
    keys = nn(lat, wk_ref[...]).astype(bf16)
    vals = nn(lat, wv_ref[...]).astype(bf16)
    rope = fold(rope_ref[...])
    for h, out in enumerate((ka_ref, kb_ref)):
        out[0:ROWS, :] = keys[:, h * NOPE : (h + 1) * NOPE]
        out[ROWS : 2 * ROWS, :] = vals[:, h * VDIM : (h + 1) * VDIM]
        out[2 * ROWS : KMSG, :] = rope
        out[KMSG:MSG, :] = jnp.zeros((MSG - KMSG, 128), bf16)
    for d, out in zip(SHIFTS, (z1_ref, z2_ref, z3_ref)):
        up = lax.rem(a + d + SIDE, SIDE) > a

        @pl.when(up)
        def _():
            out[...] = ka_ref[...]

        @pl.when(jnp.logical_not(up))
        def _():
            out[...] = qb_ref[...]


def attn_body(*refs):
    xq = refs[0:4]
    xk = refs[4:8]
    ka, qb = refs[8:10]
    zm = refs[10:13]
    own_dq, own_dk, own_dv = refs[13:16]
    out_xq = refs[16:19]
    out_xk = refs[19:22]
    out_z = refs[22:25]
    qcat, dout, lse_s, del_s, kcat, kcat_t, vals, dq, dk, dv = refs[25:]
    a, b = place()

    def take_q(i, m):
        qcat[i, :, :NOPE] = m[0:ROWS, :]
        qcat[i, :, NOPE:WIDTH] = unfold(m[2 * ROWS : KMSG, :])
        dout[i] = m[ROWS : 2 * ROWS, :]
        rows = m[KMSG:MSG, :].astype(f32)

        def joined(at):
            n = ROWS // 128
            parts = [jnp.concatenate([rows[at + n * k + j : at + n * k + j + 1] for j in range(n)], axis=1) for k in range(3)]
            return parts[0] + (parts[1] + parts[2])

        lse_s[i] = jnp.broadcast_to(joined(0), (8, ROWS))
        del_s[i] = jnp.broadcast_to(joined(12), (8, ROWS))

    def take_k(i, m):
        rope = unfold(m[2 * ROWS : KMSG, :])
        nope = m[0:ROWS, :]
        kcat[i, :, :NOPE] = nope
        kcat[i, :, NOPE:WIDTH] = rope
        kcat_t[i, :NOPE, :] = nope.T
        kcat_t[i, NOPE:, :] = rope.T
        vals[i] = m[ROWS : 2 * ROWS, :]

    dq[...] = jnp.zeros_like(dq)
    dk[...] = jnp.zeros_like(dk)
    dv[...] = jnp.zeros_like(dv)
    for s in range(4):
        take_q(s, xq[s])
        take_k(4 + s, xk[s])
    take_k(0, ka)
    take_q(4, qb)
    for n, d in enumerate(SHIFTS):
        lower = lax.rem(a - d + SIDE, SIDE) < a
        pl.when(lower)(functools.partial(take_k, n + 1, zm[n]))
        pl.when(jnp.logical_not(lower))(functools.partial(take_q, n + 5, zm[n]))

    def pair(qi, ki, diagonal):
        q = qcat[qi]
        k = kcat[ki]
        g = dout[qi]
        v = vals[ki]
        st = nt(k, q)
        pt = jnp.exp2(st * (SCALE * LOG2E) - lse_s[qi, 0:1, :])
        if diagonal:
            kpos = lax.broadcasted_iota(jnp.int32, pt.shape, 0)
            qpos = lax.broadcasted_iota(jnp.int32, pt.shape, 1)
            pt = jnp.where(kpos <= qpos, pt, 0.0)
        dpt = nt(v, g)
        dst = (pt * (dpt - del_s[qi, 0:1, :])).astype(bf16)
        dv[ki] += nn(pt.astype(bf16), g)
        dk[ki] += nn(dst, q)
        dq[qi] += nn(kcat_t[ki], dst)

    pair(0, 0, True)
    pair(4, 4, True)

    def step(p, carry):
        s = lax.rem(p, SIDE)
        u = lax.div(p, SIDE)
        shift_s = jnp.where(s == 3, 2, jnp.where(s == 2, -1, s))
        shift_u = jnp.where(u == 3, 2, jnp.where(u == 2, -1, u))
        from_x = lax.rem(b - shift_s + SIDE, SIDE)
        from_z = lax.rem(a - shift_u + SIDE, SIDE)
        first = jnp.where(u == 0, from_x > b, from_z < a)
        qi = jnp.where(first, s, 4 + u)
        ki = jnp.where(first, u, 4 + s)
        pair(qi, ki, False)
        return carry

    lax.fori_loop(1, SIDE * SIDE, step, 0)

    def put_k(out, i):
        out[0:ROWS, :] = (dk[i, :, :NOPE] * SCALE).astype(bf16)
        out[ROWS : 2 * ROWS, :] = dv[i].astype(bf16)
        out[2 * ROWS : KMSG, :] = fold((dk[i, :, NOPE:WIDTH] * SCALE).astype(bf16))

    def put_zq(out, i):
        for j in range(ROWS // 128):
            out[WIDTH * j : WIDTH * (j + 1), :] = (dq[i, :, 128 * j : 128 * (j + 1)] * SCALE).astype(bf16)
        out[WIDTH * 4 : KMSG, :] = jnp.zeros((KMSG - WIDTH * 4, 128), bf16)

    for n, d in enumerate(SHIFTS):
        out_xq[n][...] = (dq[n + 1] * SCALE).astype(bf16)
        put_k(out_xk[n], n + 5)
        lower = lax.rem(a - d + SIDE, SIDE) < a
        pl.when(lower)(functools.partial(put_k, out_z[n], n + 1))
        pl.when(jnp.logical_not(lower))(functools.partial(put_zq, out_z[n], n + 5))
    for h in range(2):
        own_dq[h] = dq[4 * h] * SCALE
        own_dk[h] = dk[4 * h] * SCALE
        own_dv[h] = dv[4 * h]


def key_side_body(*refs):
    dk_ref, dv_ref = refs[0:2]
    rx = refs[2:5]
    rz = refs[5:8]
    lat_ref, wk_ref, wv_ref = refs[8:11]
    keep_ref, send_ref, wv_own = refs[11:14]
    wv_out = refs[14:17]
    dkb, dvb, drope, dwv = refs[17:]
    a, b = place()
    core = lax.rem(lax.axis_index("tp"), 2)
    drope_sum = None
    for h in range(2):
        k = dk_ref[h, :, :NOPE]
        v = dv_ref[h]
        r = dk_ref[h, :, NOPE:WIDTH]
        for n, d in enumerate(SHIFTS):
            m = (rz, rx)[h][n]
            mk = m[0:ROWS, :].astype(f32)
            mv = m[ROWS : 2 * ROWS, :].astype(f32)
            mr = unfold(m[2 * ROWS : KMSG, :]).astype(f32)
            if h == 0:
                up = lax.rem(a + d + SIDE, SIDE) > a
                mk, mv, mr = (jnp.where(up, t, 0.0) for t in (mk, mv, mr))
            k, v, r = (k + mk, v + mv, r + mr)
        dkb[:, h * NOPE : (h + 1) * NOPE] = k.astype(bf16)
        dvb[:, h * VDIM : (h + 1) * VDIM] = v.astype(bf16)
        drope_sum = r if drope_sum is None else drope_sum + r
    drope[:, 0:ROPE] = drope_sum
    drope[:, ROPE:] = jnp.zeros((ROWS, 128 - ROPE), f32)
    half = ROWS // 2
    for out, at in ((keep_ref, core * half), (send_ref, (1 - core) * half)):
        rows = pl.ds(pl.multiple_of(at, half), half)
        part = nt(dkb[rows, :], wk_ref[...]) + nt(dvb[rows, :], wv_ref[...])
        out[:, 0:LATENT] = part.astype(out.dtype)
        out[:, LATENT:] = drope[rows, :].astype(out.dtype)
    dwv[...] = tn(lat_ref[...], dvb[...])
    for out, d in zip((wv_own, *wv_out), (0, *SHIFTS)):
        to_x = lax.rem(b + d + SIDE, SIDE)
        for z in range(SIDE):
            at = pl.multiple_of(64 * (SIDE * z + to_x), 64)
            out[64 * z : 64 * (z + 1), :] = dwv[pl.ds(at, 64), :].astype(out.dtype)


def weight_mid_body(own, r1, r2, r3, keep, o1, o2, o3, acc):
    a, _ = place()
    acc[...] = own[...] + r1[...].astype(f32) + r2[...].astype(f32) + r3[...].astype(f32)
    for out, d in zip((keep, o1, o2, o3), (0, *SHIFTS)):
        at = pl.multiple_of(64 * lax.rem(a + d + SIDE, SIDE), 64)
        out[...] = acc[pl.ds(at, 64), :].astype(out.dtype)


def latent_mid_body(own, r1, keep, o1, o2, o3, acc):
    y = lax.div(lax.axis_index("tp"), 2)
    acc[...] = own[...] + r1[...].astype(f32)
    for out, d in zip((keep, o1, o2, o3), (0, *SHIFTS)):
        at = pl.multiple_of(64 * lax.rem(y + d + SIDE, SIDE), 64)
        out[...] = acc[pl.ds(at, 64), :].astype(out.dtype)


def sum_body(own, r1, r2, r3, out):
    total = own[...] + r1[...].astype(f32) + r2[...].astype(f32) + r3[...].astype(f32)
    out[...] = total.astype(out.dtype)


def spread_body(mine_ref, other_ref, lat_ref, rope_ref):
    t = lax.axis_index("tp")
    y = lax.div(t, 2)
    core = lax.rem(t, 2)
    for src, c in ((mine_ref, core), (other_ref, 1 - core)):
        for n, d in enumerate((0, *SHIFTS)):
            at = pl.multiple_of(256 * c + 64 * lax.rem(y - d + SIDE, SIDE), 64)
            piece = src[64 * n : 64 * (n + 1), :]
            lat_ref[pl.ds(at, 64), :] = piece[:, 0:LATENT].astype(f32)
            rope_ref[pl.ds(at, 64), :] = piece[:, LATENT : LATENT + ROPE].astype(f32)


def query_side_body(dq_ref, x1, x2, x3, z1, z2, z3, out):
    a, _ = place()
    first = dq_ref[0] + x1[...].astype(f32) + x2[...].astype(f32) + x3[...].astype(f32)
    second = dq_ref[1]
    for d, m in zip(SHIFTS, (z1, z2, z3)):
        down = lax.rem(a + d + SIDE, SIDE) < a
        got = jnp.concatenate([m[WIDTH * j : WIDTH * (j + 1), :] for j in range(ROWS // 128)], axis=1)
        second = second + jnp.where(down, got.astype(f32), 0.0)
    both = jnp.concatenate([first, second], axis=0)
    out[...] = both.T.astype(bf16)


def call(body, outs, scratch=(), name=None):
    shapes = tuple(jax.ShapeDtypeStruct(s, t) for s, t in outs)
    return pl.pallas_call(
        body,
        out_shape=shapes,
        scratch_shapes=[pltpu.VMEM(s, t) for s, t in scratch],
        compiler_params=pltpu.CompilerParams(vmem_limit_bytes=60 * 1024 * 1024),
        name=name,
    )


def per_device(queries, latent, rope_key, key_weight, value_weight, log_sums, attn_out, out_grad):
    msg = ((MSG, 128), bf16)
    kmsg = ((KMSG, 128), bf16)
    qa, qb = call(prep_q_body, (msg, msg), name="prep_q")(queries, attn_out, out_grad, log_sums)
    got_xq = [lax.ppermute(qa, "sp", x_perm(d)) for d in SHIFTS]
    ka, kb, *zs = call(prep_k_body, (msg,) * 5, name="prep_k")(
        latent, key_weight, value_weight, rope_key, qb
    )
    got_xk = [lax.ppermute(kb, "sp", x_perm(d)) for d in SHIFTS]
    got_z = [lax.ppermute(m, "sp", z_perm(d)) for m, d in zip(zs, SHIFTS)]

    dq_t = ((2, WIDTH, ROWS), f32)
    outs = call(
        attn_body,
        (dq_t, ((2, ROWS, WIDTH), f32), ((2, ROWS, VDIM), f32))
        + (((WIDTH, ROWS), bf16),) * 3
        + (kmsg,) * 6,
        (
            ((8, ROWS, WIDTH), bf16),
            ((8, ROWS, VDIM), bf16),
            ((8, 8, ROWS), f32),
            ((8, 8, ROWS), f32),
            ((8, ROWS, WIDTH), bf16),
            ((8, WIDTH, ROWS), bf16),
            ((8, ROWS, VDIM), bf16),
            ((8, WIDTH, ROWS), f32),
            ((8, ROWS, WIDTH), f32),
            ((8, ROWS, VDIM), f32),
        ),
        name="attn",
    )(qa, *got_xq, kb, *got_xk, ka, qb, *got_z)
    own_dq, own_dk, own_dv = outs[0:3]
    back_xk = [lax.ppermute(m, "sp", x_perm(-d)) for m, d in zip(outs[6:9], SHIFTS)]
    back_z = [lax.ppermute(m, "sp", z_perm(-d)) for m, d in zip(outs[9:12], SHIFTS)]
    back_xq = [lax.ppermute(m, "sp", x_perm(-d)) for m, d in zip(outs[3:6], SHIFTS)]

    half = ROWS // 2
    keep, send, wv_own, *wv_send = call(
        key_side_body,
        (((half, OUTW), f32), ((half, OUTW), bf16), ((256, 256), f32)) + (((256, 256), bf16),) * 3,
        (
            ((ROWS, 2 * NOPE), bf16),
            ((ROWS, 2 * VDIM), bf16),
            ((ROWS, 128), f32),
            ((LATENT, 2 * VDIM), f32),
        ),
        name="key_side",
    )(own_dk, own_dv, *back_xk, *back_z, latent, key_weight, value_weight)
    other = lax.ppermute(send, "tp", core_perm())
    wv_got = [lax.ppermute(m, "sp", x_perm(d)) for m, d in zip(wv_send, SHIFTS)]

    piece = ((64, OUTW), bf16)
    l_own, *l_send = call(
        latent_mid_body, (((64, OUTW), f32),) + (piece,) * 3, (((half, OUTW), f32),), name="latent_mid"
    )(keep, other)
    l_got = [lax.ppermute(m, "tp", y_perm(d)) for m, d in zip(l_send, SHIFTS)]

    w_own, *w_send = call(
        weight_mid_body,
        (((64, 256), f32),) + (((64, 256), bf16),) * 3,
        (((256, 256), f32),),
        name="weight_mid",
    )(wv_own, *wv_got)
    w_got = [lax.ppermute(m, "sp", z_perm(d)) for m, d in zip(w_send, SHIFTS)]

    (l_sum,) = call(sum_body, (piece,), name="latent_sum")(l_own, *l_got)
    l_all = [lax.ppermute(l_sum, "tp", y_perm(d)) for d in SHIFTS]
    (d_queries,) = call(query_side_body, (((ROWS, 2 * WIDTH), bf16),), name="query_side")(
        own_dq, *back_xq, *back_z
    )
    (d_value_weight,) = call(sum_body, (((64, 256), f32),), name="weight_sum")(w_own, *w_got)
    mine = jnp.concatenate([l_sum, *l_all], axis=0)
    theirs = lax.ppermute(mine, "tp", core_perm())
    d_latent, d_rope = call(
        spread_body, (((ROWS, LATENT), f32), ((ROWS, ROPE), f32)), name="spread"
    )(mine, theirs)
    return (d_queries, d_latent, d_rope, d_value_weight)


def solution(mesh):
    placed = (
        P("sp", "tp"),
        P("sp", None),
        P("sp", None),
        P(None, "tp"),
        P(None, "tp"),
        P("tp", "sp"),
        P("sp", "tp"),
        P("sp", "tp"),
    )
    return jax.shard_map(
        per_device,
        mesh=mesh,
        in_specs=placed,
        out_specs=(P("sp", "tp"), P("sp", None), P("sp", None), P("sp", "tp")),
        check_vma=False,
    )
```
